128 devices in a mesh: sp: 32 (over z, y, core), tp: 4 (over x).
Axes of the slice: x: 4, y: 4, z: 4, core: 2. Of those that a mesh axis runs over, the one named last changes fastest.
Arguments:
- query: bfloat16 [49152, 512], P('sp', 'tp'), may hold values from -6 to 6
- key_rows: bfloat16 [49152, 512], P('sp', 'tp'), may hold values from -6 to 6
- value: bfloat16 [49152, 1024], P('sp', 'tp'), may hold values from -6 to 6
- in_gate: float32 [2, 8, 49152], P(None, 'tp', 'sp'), may hold values from -6 to 250
- forget_pre: float32 [2, 8, 49152], P(None, 'tp', 'sp'), may hold values from 0.3 to 12
- out_gate: bfloat16 [49152, 1024], P('sp', 'tp'), may hold values from -6 to 6
- head_gain: bfloat16 [1024], P('tp'), may hold values from 0.099609375 to 1.8984375
- out_weight: bfloat16 [1024, 2048], P('tp'), may hold values from -0.25 to 0.25
- stream: bfloat16 [49152, 2048], P('sp', 'tp'), may hold values from -16 to 16
- norm_gain: bfloat16 [2048], P('tp'), may hold values from 0.099609375 to 1.8984375
- gate_weight: bfloat16 [2048, 5632], P('sp', 'tp'), may hold values from -0.125 to 0.125
- up_weight: bfloat16 [2048, 5632], P('sp', 'tp'), may hold values from -0.125 to 0.125
- down_weight: bfloat16 [2048, 5632], P('sp', 'tp'), may hold values from -0.15625 to 0.15625
Outputs:
- layer_out: bfloat16 [49152, 2048], P('sp', 'tp')
The draws below stay inside these ranges and needn't reach their ends.
All inputs are finite; a program needn't handle non-finite values.
Results may differ from the reference program's by a relative error of at most 0.04.
Values may be sent and summed in bfloat16 or wider, within the bound.
A program may use at most 128 MiB of HBM per device.

```python
import jax
import jax.numpy as jnp
from jax import lax

D = 2048
MEMORY_HEADS = 8
DK = 64
DV = 128
FF = 5632
BLOCK = 128
TOK_DEV = 1536
SEQUENCE_TOKENS = 49152
N_TP = 4


def draw_in_gate(key, part):
    random_subkeys = jax.random.split(jax.random.fold_in(key, 11), 1)
    return jnp.clip(1.5 * jax.random.normal(random_subkeys[0], (2, MEMORY_HEADS, SEQUENCE_TOKENS), jnp.float32), -6.0, 6.0)


def draw_forget_pre(key, part):
    random_subkeys = jax.random.split(jax.random.fold_in(key, 23), 5)
    slow_share = 0.5
    slow = jax.random.uniform(random_subkeys[0], (2, MEMORY_HEADS, 1), jnp.float32) < slow_share
    spans = SEQUENCE_TOKENS // TOK_DEV
    factor = jnp.exp(jax.random.uniform(random_subkeys[1], (2, MEMORY_HEADS, spans), jnp.float32, -0.6931, 0.6931))
    factor = jnp.repeat(factor, TOK_DEV, axis=2)
    noise = 0.7 * jnp.clip(jax.random.normal(random_subkeys[2], (2, MEMORY_HEADS, SEQUENCE_TOKENS), jnp.float32), -2.5, 2.5)
    slow_pre = jnp.log(SEQUENCE_TOKENS / (0.6 * factor)) + noise
    fast_pre = jnp.log(50.0 / factor) + noise
    final_output = jnp.clip(jnp.where(slow, slow_pre, fast_pre), 0.3, 12.0)
    spike_list = jax.random.randint(random_subkeys[3], (2, MEMORY_HEADS, 3), 0, SEQUENCE_TOKENS)
    token_offset = jnp.arange(SEQUENCE_TOKENS)[None, None, None, :]
    flagged_entries = jnp.any(token_offset == spike_list[..., None], axis=2)
    spike_value = jax.random.uniform(random_subkeys[4], (2, MEMORY_HEADS, SEQUENCE_TOKENS), jnp.float32, 0.3, 1.5)
    return jnp.where(flagged_entries, spike_value, final_output)


def draw_stream(key, part):
    random_subkeys = jax.random.split(jax.random.fold_in(key, 37), 2)
    columns = jnp.arange(D, dtype=jnp.float32) / D
    rowdraw = jax.random.uniform(random_subkeys[1], (SEQUENCE_TOKENS, 1), jnp.float32)
    base = jnp.clip(jax.random.normal(random_subkeys[0], (SEQUENCE_TOKENS, D), jnp.float32), -4.0, 4.0)
    column_scale = jnp.exp(jnp.log(4.0) * (columns - 0.5))
    row_scale = jnp.exp(jnp.log(10.0) * (rowdraw - 0.7))
    return (base * row_scale * column_scale[None, :]).astype(jnp.bfloat16)


def raised(drawn, key, source, target, blocks, factor):
    def block_of(axis_at):
        return (jnp.arange(drawn.shape[axis_at]) // (drawn.shape[axis_at] // blocks)).reshape((-1,) + (1,) * (drawn.ndim - 1 - axis_at))

    first = jax.random.permutation(key, blocks)[block_of(target)]
    second = (block_of(target) + blocks // 2) % blocks
    return jnp.where((block_of(source) == first) | (block_of(source) == second), factor * drawn, drawn)


def block_scale(own_key, shape, cuts, least, largest):
    gain = 1.0
    for dim, blocks in cuts:
        draws = jax.random.uniform(jax.random.fold_in(jax.random.fold_in(own_key, 6), dim), (blocks,), jnp.float32, least / len(cuts), largest / len(cuts))
        gain = gain * jnp.repeat(jnp.exp(draws), shape[dim] // blocks).reshape((-1,) + (1,) * (len(shape) - 1 - dim))
    return gain


def scatter_about(rng, shape, scale, reach, cuts=(), kind=jnp.bfloat16):
    values = jax.random.normal(rng, shape, jnp.float32) * scale
    if len(cuts) > 0:
        values = block_scale(rng, shape, cuts, -0.22, 0.18) * values
    return jnp.clip(values, min=-reach, max=reach).astype(kind)


def gaussian_with(own_key, extent, spread, most, shards, heavy, held_as=jnp.bfloat16):
    values = spread * jax.random.normal(own_key, extent, jnp.float32)
    if shards:
        values = values * block_scale(own_key, extent, shards, -0.22, 0.18)
    return jnp.clip(raised(values, jax.random.fold_in(own_key, 3), *heavy), -most, most).astype(held_as)


def setup_inputs(seed: int = 0) -> dict:
    arg_keys = jax.random.split(jax.random.key(seed), 14)
    return {
        "query": scatter_about(arg_keys[0], (SEQUENCE_TOKENS, MEMORY_HEADS * DK), 1.0, 6.0, ((0, 32), (1, 4))),
        "key_rows": scatter_about(arg_keys[1], (SEQUENCE_TOKENS, MEMORY_HEADS * DK), 1.0, 6.0, ((0, 32), (1, 4))),
        "value": scatter_about(arg_keys[2], (SEQUENCE_TOKENS, MEMORY_HEADS * DV), 1.0, 6.0, ((0, 32), (1, 4))),
        "in_gate": draw_in_gate(jax.random.fold_in(arg_keys[13], 71), 0),
        "forget_pre": draw_forget_pre(jax.random.fold_in(arg_keys[13], 71), 0),
        "out_gate": scatter_about(arg_keys[5], (SEQUENCE_TOKENS, MEMORY_HEADS * DV), 1.5, 6.0, ((0, 32), (1, 4))),
        "head_gain": jnp.clip(1.0 + 0.18 * jax.random.normal(arg_keys[6], (MEMORY_HEADS * DV,), jnp.float32), 0.099609375, 1.8984375).astype(jnp.bfloat16),
        "out_weight": gaussian_with(arg_keys[7], (MEMORY_HEADS * DV, D), (MEMORY_HEADS * DV) ** -0.5, 0.25, ((0, 4),), (0, 1, 4, 2.0)),
        "stream": draw_stream(jax.random.fold_in(arg_keys[13], 71), 0),
        "norm_gain": jnp.clip(1.0 + 0.18 * jax.random.normal(arg_keys[9], (D,), jnp.float32), 0.099609375, 1.8984375).astype(jnp.bfloat16),
        "gate_weight": scatter_about(arg_keys[10], (D, FF), D ** -0.5, 0.125, ((0, 32), (1, 4))),
        "up_weight": scatter_about(arg_keys[11], (D, FF), D ** -0.5, 0.125, ((0, 32), (1, 4))),
        "down_weight": gaussian_with(arg_keys[12], (D, FF), FF ** -0.5, 0.15625, ((0, 32), (1, 4)), (1, 0, 32, 2.75)),
    }


HIGHEST = lax.Precision.HIGHEST
EPSILON = 1e-06

def direction(queries, keys, values, input_gates, forgets):
    head_count = queries.shape[0]
    block_count = queries.shape[1] // BLOCK

    def blocks(item):
        shaped = item.reshape((head_count, block_count, BLOCK) + item.shape[2:])
        return jnp.moveaxis(shaped, 1, 0)
    causal = jnp.tril(jnp.ones((BLOCK, BLOCK), dtype=bool))

    def step(carry, pieces):
        matrix, normer, stable = carry
        query_part, key_part, value_part, gate_part, forget_part = pieces
        cumulative = jnp.cumsum(forget_part, axis=-1)
        decay_log = jnp.where(causal, cumulative[:, :, None] - cumulative[:, None, :] + gate_part[:, None, :], -jnp.inf)
        carry_log = cumulative + stable[:, None]
        row_peak = jnp.maximum(carry_log, lax.optimization_barrier(jnp.max(decay_log, axis=-1)))
        scores = jnp.einsum('hjd,hsd->hjs', query_part, key_part, precision=HIGHEST) * jnp.exp(decay_log - row_peak[:, :, None])
        carried = jnp.exp(carry_log - row_peak)
        numerator = jnp.einsum('hjs,hsv->hjv', scores, value_part, precision=HIGHEST) + carried[:, :, None] * jnp.einsum('hvd,hjd->hjv', matrix, query_part, precision=HIGHEST)
        denominator = lax.optimization_barrier(jnp.sum(scores, axis=-1)) + carried * jnp.einsum('hd,hjd->hj', normer, query_part, precision=HIGHEST)
        output = numerator / jnp.maximum(jnp.abs(denominator), jnp.exp(-row_peak))[:, :, None]
        block_total = cumulative[:, -1]
        weight_log = block_total[:, None] - cumulative + gate_part
        new_stable = jnp.maximum(block_total + stable, lax.optimization_barrier(jnp.max(weight_log, axis=-1)))
        shrink = jnp.exp(block_total + stable - new_stable)
        weight = jnp.exp(weight_log - new_stable[:, None])
        new_matrix = shrink[:, None, None] * matrix + jnp.einsum('hsv,hsd->hvd', weight[:, :, None] * value_part, key_part, precision=HIGHEST)
        new_normer = shrink[:, None] * normer + jnp.einsum('hs,hsd->hd', weight, key_part, precision=HIGHEST)
        return ((new_matrix, new_normer, new_stable), output)
    initial = (jnp.zeros((head_count, values.shape[2], queries.shape[2]), jnp.float32), jnp.zeros((head_count, queries.shape[2]), jnp.float32), jnp.zeros((head_count,), jnp.float32))
    _, results = lax.scan(step, initial, (blocks(queries), blocks(keys), blocks(values), blocks(input_gates), blocks(forgets)))
    return jnp.moveaxis(results, 0, 1).reshape(head_count, -1, values.shape[2])

def reverse_time(item):
    return jnp.flip(item, axis=1)

def reference(query, key_rows, value, in_gate, forget_pre, out_gate, head_gain, out_weight, stream, norm_gain, gate_weight, up_weight, down_weight):
    length = query.shape[0]

    def split_heads(item, width):
        return jnp.transpose(item.astype(jnp.float32).reshape(length, MEMORY_HEADS, width), (1, 0, 2))
    queries = split_heads(query, DK) * DK ** (-0.5)
    keys = split_heads(key_rows, DK)
    values = split_heads(value, DV)
    gates_in = in_gate.astype(jnp.float32)
    forgets = jax.nn.log_sigmoid(forget_pre.astype(jnp.float32))
    forward = direction(queries, keys, values, gates_in[0], forgets[0])
    backward = reverse_time(direction(reverse_time(queries), reverse_time(keys), reverse_time(values), reverse_time(gates_in[1]), reverse_time(forgets[1])))
    summed = forward + backward
    head_normed = summed * lax.rsqrt(lax.optimization_barrier(jnp.mean(summed * summed, axis=-1, keepdims=True)) + EPSILON)
    merged = jnp.transpose(head_normed, (1, 0, 2)).reshape(length, MEMORY_HEADS * DV)
    gated = (merged * head_gain.astype(jnp.float32) * jax.nn.sigmoid(out_gate.astype(jnp.float32))).astype(jnp.bfloat16)
    group_width = MEMORY_HEADS * DV // N_TP
    mixed_sum = jnp.zeros((length, D), jnp.float32)
    for group_index in range(N_TP):
        lower = group_index * group_width
        partial_value = jnp.dot(gated[:, lower:lower + group_width], out_weight[lower:lower + group_width], preferred_element_type=jnp.float32)
        mixed_sum = mixed_sum + lax.optimization_barrier(partial_value.astype(jnp.bfloat16)).astype(jnp.float32)
    residual = stream.astype(jnp.float32) + mixed_sum
    normed = (residual * lax.rsqrt(lax.optimization_barrier(jnp.mean(residual * residual, axis=-1, keepdims=True)) + EPSILON) * norm_gain.astype(jnp.float32)).astype(jnp.bfloat16)
    hidden_width = FF // N_TP
    feed_sum = jnp.zeros((length, D), jnp.float32)
    for group_index in range(N_TP):
        lower = group_index * hidden_width
        gate_pre = jnp.dot(normed, gate_weight[:, lower:lower + hidden_width], preferred_element_type=jnp.float32)
        up_value = jnp.dot(normed, up_weight[:, lower:lower + hidden_width], preferred_element_type=jnp.float32)
        hidden = (jax.nn.silu(gate_pre) * up_value).astype(jnp.bfloat16)
        partial_value = jnp.dot(hidden, down_weight[:, lower:lower + hidden_width].T, preferred_element_type=jnp.float32)
        feed_sum = feed_sum + lax.optimization_barrier(partial_value.astype(jnp.bfloat16)).astype(jnp.float32)
    return (residual + feed_sum).astype(jnp.bfloat16)
```

```python
import functools

import jax
import jax.numpy as jnp
from jax import lax
from jax.experimental import pallas as pl
from jax.experimental.pallas import tpu as pltpu
from jax.sharding import PartitionSpec as P

D = 2048
EPSILON = 1e-06
VERY_LOW = -1e30
F32 = jnp.float32
BF16 = jnp.bfloat16
ROWS = 256
VMEM_MAX = 60 * 1024 * 1024


def dot(a, b):
    return jnp.dot(a, b, preferred_element_type=F32)


def dot_t(a, b):
    return lax.dot_general(a, b, (((1,), (1,)), ((), ())), preferred_element_type=F32)


def lane_scan(x, op, neutral, backward):
    n = x.shape[1]
    lane = lax.broadcasted_iota(jnp.int32, x.shape, 1)
    step = 1
    while step < n:
        if backward:
            moved, ok = pltpu.roll(x, n - step, 1), lane < n - step
        else:
            moved, ok = pltpu.roll(x, step, 1), lane >= step
        x = op(x, jnp.where(ok, moved, neutral))
        step *= 2
    return x


def summarise(k_ref, v_ref, in_ref, fg_ref, gates_ref, st_ref):
    n = k_ref.shape[0]
    pre = jnp.concatenate([fg_ref[0], fg_ref[1], fg_ref[0], fg_ref[1]], axis=0)
    gate = jnp.concatenate([in_ref[0], in_ref[1], in_ref[0], in_ref[1]], axis=0)
    u = jnp.exp(-jnp.abs(pre))
    w = 1.0 + u
    tail = jnp.where(w == 1.0, u, jnp.log(w) * u / jnp.where(w == 1.0, 1.0, w - 1.0))
    logf = jnp.minimum(pre, 0.0) - tail
    row = lax.broadcasted_iota(jnp.int32, logf.shape, 0)
    ahead = (row % 4) < 2
    b = jnp.where(
        ahead,
        lane_scan(logf, jnp.add, 0.0, False),
        lane_scan(logf, jnp.add, 0.0, True),
    )
    a = gate - b
    top = jnp.where(
        ahead,
        lane_scan(a, jnp.maximum, VERY_LOW, False),
        lane_scan(a, jnp.maximum, VERY_LOW, True),
    )
    gates_ref[0:8] = a
    gates_ref[8:16] = top
    gates_ref[16:24] = b
    peak = jnp.where(ahead[:, :1], top[:, n - 1 :], top[:, :1])
    total = jnp.where(ahead[:, :1], b[:, n - 1 :], b[:, :1])
    st_ref[272:280] = jnp.broadcast_to(total + peak, (8, 128))
    st_ref[280:288] = jnp.broadcast_to(total, (8, 128))
    weight = jnp.exp(a - peak)
    kt = jnp.transpose(k_ref[...].astype(F32))
    ones = jnp.ones((n, 128), BF16)
    norms = [[], []]
    for h in range(2):
        kh = kt[64 * h : 64 * h + 64]
        lhs = jnp.concatenate([kh * weight[h : h + 1], kh * weight[2 + h : 3 + h]], axis=0)
        vx = jnp.concatenate([v_ref[:, 128 * h : 128 * h + 128], ones], axis=1)
        made = dot(lhs.astype(BF16), vx)
        for d in range(2):
            st_ref[136 * d + 64 * h : 136 * d + 64 * h + 64] = made[64 * d : 64 * d + 64, :128]
            norms[d].append(made[64 * d : 64 * d + 64, 128:])
    for d in range(2):
        turned = jnp.transpose(jnp.concatenate(norms[d], axis=0))
        st_ref[136 * d + 128 : 136 * d + 136] = turned[:8]


def merged(first, second):
    m1, m2, total = first[0], second[0], second[1]
    top = jnp.maximum(m1 + total, m2)
    return top, jnp.exp(m1 + total - top), jnp.exp(m2 - top)


def spread_rows(factor, d):
    heads = [jnp.where(d == 0, factor[h : h + 1], factor[2 + h : 3 + h]) for h in range(2)]
    rows = jnp.concatenate([jnp.broadcast_to(x, (64, 128)) for x in heads], axis=0)
    lane = lax.broadcasted_iota(jnp.int32, (8, 128), 1)
    return rows, jnp.where(lane < 64, heads[0], heads[1])


MESH = pl.DeviceIdType.MESH
TP = 4
CHUNK = 384
HALF = CHUNK // 2
WIDE = 512
HID = 1408
PART = CHUNK // TP
STEPS = TP
TINY = 1e-35


def peer(index):
    return {"tp": lax.rem(index, TP)}


def greet(devices):
    barrier = pltpu.get_barrier_semaphore()
    for to in devices:
        pl.semaphore_signal(barrier, inc=1, device_id=to, device_id_type=MESH)
    pl.semaphore_wait(barrier, len(devices))


def remote(src, dst, send, recv, to):
    return pltpu.make_async_remote_copy(
        src_ref=src, dst_ref=dst, send_sem=send, recv_sem=recv, device_id=to, device_id_type=MESH
    )


def attend_local(q_ref, k_ref, v_ref, gates_ref, num_ref, den_ref, vx_ref, between):
    n = q_ref.shape[0]
    for h in range(2):
        vx_ref[h, :, :128] = v_ref[:, 128 * h : 128 * h + 128]
        vx_ref[h, :, 128:] = jnp.ones((n, 128), BF16)
    a, top = gates_ref[0:8], gates_ref[8:16]
    lane = lax.broadcasted_iota(jnp.int32, (ROWS, 128), 1)
    col = lax.broadcasted_iota(jnp.int32, (ROWS, ROWS), 1)
    row = lax.broadcasted_iota(jnp.int32, (ROWS, ROWS), 0)
    below, above = col <= row, col >= row
    for j in range(n // ROWS):
        at = j * ROWS
        qs = q_ref[at : at + ROWS].astype(F32) * 0.125
        for h in range(2):
            qh = jnp.where((lane < 64) == (h == 0), qs, 0.0).astype(BF16)
            scores = dot_t(qh, k_ref[...])
            for d in range(2):
                r = 2 * d + h
                first, last = (0, at + ROWS) if d == 0 else (at, n)
                tops = jnp.transpose(
                    jnp.broadcast_to(top[r : r + 1, at : at + ROWS], (128, ROWS))
                )
                reach = (last - first) // 128
                logs = a[r : r + 1, first:last] - jnp.concatenate([tops] * reach, axis=1)
                if d == 0:
                    edge = jnp.where(below, logs[:, at:], VERY_LOW)
                    logs = edge if j == 0 else jnp.concatenate([logs[:, :at], edge], axis=1)
                else:
                    edge = jnp.where(above, logs[:, :ROWS], VERY_LOW)
                    logs = (
                        edge
                        if last == at + ROWS
                        else jnp.concatenate([edge, logs[:, ROWS:]], axis=1)
                    )
                weighed = (scores[:, first:last] * jnp.exp(logs)).astype(BF16)
                acc = dot(weighed, vx_ref[h, first:last])
                num_ref[at : at + ROWS, 128 * r : 128 * r + 128] = acc[:, :128]
                den_ref[at : at + ROWS, 128 * r : 128 * r + 128] = acc[:, 128:]
        between(j)


def attend_rows(at, q_ref, gates_ref, og_ref, gain_ref, num_ref, den_ref, out_ref, rhs, m0):
    rows = pl.ds(at, CHUNK)
    own_top = gates_ref[8:16, rows]
    top = jnp.maximum(own_top, m0[:, :1])
    share = jnp.exp(own_top - top)
    keep = jnp.exp(m0[:, :1] - top)
    floor = jnp.maximum(jnp.exp(-(gates_ref[16:24, rows] + top)), TINY)
    lane = lax.broadcasted_iota(jnp.int32, (CHUNK, 128), 1)
    qs = q_ref[rows].astype(F32) * 0.125

    def column(of, r):
        return jnp.transpose(jnp.broadcast_to(of[r : r + 1], (128, CHUNK)))

    for h in range(2):
        qh = jnp.where((lane < 64) == (h == 0), qs, 0.0).astype(BF16)
        q2 = jnp.concatenate([qh, qh], axis=1)
        total = None
        for d in range(2):
            r = 2 * d + h
            lanes = slice(128 * r, 128 * r + 128)
            state = dot(q2, rhs[d])
            kept, part = column(keep, r), column(share, r)
            acc_n = part * num_ref[rows, lanes] + kept * state[:, :128]
            acc_d = part * den_ref[rows, lanes] + kept * state[:, 128:]
            one = acc_n / jnp.maximum(jnp.abs(acc_d), column(floor, r))
            total = one if total is None else total + one
        scale = lax.rsqrt(jnp.mean(total * total, axis=1, keepdims=True) + EPSILON)
        lanes = slice(128 * h, 128 * h + 128)
        gate = og_ref[rows, lanes].astype(F32)
        out_ref[rows, lanes] = (
            total * scale * gain_ref[:, lanes].astype(F32) * (1.0 / (1.0 + jnp.exp(-gate)))
        ).astype(BF16)


def layer_kernel(
    q_ref,
    k_ref,
    v_ref,
    in_ref,
    fg_ref,
    og_ref,
    gain_ref,
    ngain_ref,
    stream_ref,
    ow_ref,
    gate_hbm,
    up_hbm,
    down_hbm,
    out_ref,
    gates_ref,
    st_ref,
    pst_ref,
    cst_ref,
    gst_ref,
    pri_ref,
    ppri_ref,
    lw_ref,
    vx_ref,
    gated_ref,
    gt_ref,
    grel_ref,
    sm_ref,
    srel_ref,
    gn_ref,
    ow_all,
    res_ref,
    own_ref,
    w_ref,
    x_ref,
    hidden_ref,
    made_ref,
    half_ref,
    next_ref,
    got_half,
    got_next,
    send,
    recv,
    ring_send,
    ring_recv,
    own_sem,
):
    me, sp = lax.axis_index("tp"), lax.axis_index("sp")
    sps = lax.axis_size("sp")
    chips = sps // 2
    depth = 2048 // sps
    quart = depth // 4
    n_y = min(TP, chips)
    n_z = chips // n_y
    core, chip = sp % 2, sp // 2
    place = core * (chips - 1 - chip) + (1 - core) * chip
    turn = 1 - 2 * core
    right, left = peer(me + 1), peer(me + 3)
    partner = {"sp": sp + turn}
    y, z = chip % n_y, chip // n_y

    def chip_at(k):
        return {"sp": 2 * lax.rem(chip + k + chips, chips) + core}

    greet(
        [peer(me + d) for d in (1, 2, 3)] + [partner] + [chip_at(k) for k in range(1, chips)]
    )
    at_right, at_left, across = (
        lax.rem(me + 1, TP),
        lax.rem(me + 3, TP),
        lax.rem(me + 2, TP),
    )
    used = [0]
    started = []

    def copy(src, dst, to):
        i = used[0]
        used[0] += 1
        return remote(src, dst, send.at[i], recv.at[i], to)

    def go(copies):
        for one in copies:
            one.start()
            started.append(one)

    def arrive(copies):
        for one in copies:
            one.wait_recv()

    def rows_of(at, start=0, size=CHUNK):
        return pl.ds(pl.multiple_of(at * CHUNK + start, HALF), size)

    low, high = pl.ds(0, HALF), pl.ds(HALF, HALF)
    cols = pl.ds(pl.multiple_of(core * 1024, 1024), 1024)

    def o_rows(at, start=0, size=256):
        return pl.ds(pl.multiple_of(at * 256 + start, 128), size)

    def exchange(source, relay_ref, target):
        return [
            copy(source.at[rows_of(across, 0, HALF)], relay_ref.at[0], right),
            copy(source.at[rows_of(across, HALF, HALF)], relay_ref.at[1], left),
            copy(source.at[rows_of(at_right)], target.at[me], right),
            copy(source.at[rows_of(at_left)], target.at[me], left),
        ], [
            copy(relay_ref.at[0], target.at[at_left, low], right),
            copy(relay_ref.at[1], target.at[at_right, high], left),
        ]

    s_first, s_next = exchange(stream_ref, srel_ref, sm_ref)
    g_first, g_next = exchange(gated_ref, grel_ref, gt_ref)
    gains = [copy(ngain_ref, gn_ref.at[me], peer(me + d)) for d in (1, 2, 3)]
    o_first = [copy(ow_ref.at[:, cols], ow_all.at[o_rows(me), cols], to) for to in (right, left)]

    def o_piece(at, start, size, to):
        piece = ow_all.at[o_rows(at, start, size), cols]
        return copy(piece, piece, to)

    o_next = [o_piece(at_left, 0, 128, right), o_piece(at_right, 128, 128, left)]
    o_over = [
        o_piece(at_left, 0, 256, partner),
        o_piece(at_right, 0, 256, partner),
        o_piece(across, 0, 128, partner),
        o_piece(across, 128, 128, partner),
    ]

    def row_at(yy, zz):
        return (2 * (zz * n_y + yy) + core) * depth

    def w_piece(row, size, to):
        piece = w_ref.at[pl.ds(pl.multiple_of(row, 16), size)]
        return copy(piece, piece, to)

    def ring_of(pos, n, axis):
        if n == 1:
            return None
        up, down = lax.rem(pos + 1, n), lax.rem(pos + n - 1, n)
        ids = [
            {"sp": (2 * (z * n_y + p) if axis == 0 else 2 * (p * n_y + y)) + core}
            for p in (up, down)
        ]
        return up, down, lax.rem(pos + 2, n), ids

    rings = [ring_of(y, n_y, 0), ring_of(z, n_z, 1)]

    def spot(axis, a, b, part):
        return (row_at(a, b) if axis == 0 else row_at(b, a)) + part * 2 * quart

    here = (y, z)
    first_out, first_on, second = [], [], []
    for part in range(2):
        axis = part
        ring, other = rings[axis], rings[1 - axis]
        pos, fixed = here[axis], here[1 - axis]
        places = [[pos]]
        if ring is not None:
            up, down, far, ids = ring
            mine = spot(axis, pos, fixed, part)
            first_out += [w_piece(mine, 2 * quart, ids[0]), w_piece(mine, 2 * quart, ids[1])]
            first_on += [
                w_piece(spot(axis, down, fixed, part), quart, ids[0]),
                w_piece(spot(axis, up, fixed, part) + quart, quart, ids[1]),
            ]
            places += [[down, up], [far]]
        stages = []
        for group in places:
            direct, onward = [], []
            if other is not None:
                up2, down2, _, ids2 = other
                for p in group:
                    row = spot(axis, p, fixed, part)
                    direct += [w_piece(row, 2 * quart, ids2[0]), w_piece(row, 2 * quart, ids2[1])]
                    onward += [
                        w_piece(spot(axis, p, down2, part), quart, ids2[0]),
                        w_piece(spot(axis, p, up2, part) + quart, quart, ids2[1]),
                    ]
            stages.append((direct, onward))
        second.append(stages)
    direct = [sum((second[p][g][0] for p in range(2) if g < len(second[p])), []) for g in range(3)]
    onward = [sum((second[p][g][1] for p in range(2) if g < len(second[p])), []) for g in range(3)]
    over = [
        w_piece(row_at(yy, zz), depth, partner) for zz in range(n_z) for yy in range(n_y)
    ]

    w_own = pl.ds(pl.multiple_of(sp * depth, 16), depth)
    loads = []
    for i in range(HID // 128):
        for j, source in enumerate((gate_hbm, up_hbm)):
            loads.append(
                (source.at[:, 128 * i : 128 * i + 128], w_ref.at[w_own, pl.ds(256 * i + 128 * j, 128)])
            )
    loads.append((down_hbm, w_ref.at[w_own, pl.ds(2 * HID, HID)]))
    loads += [
        (stream_ref.at[rows_of(me)], sm_ref.at[me]),
        (ngain_ref, gn_ref.at[me]),
        (ow_ref, ow_all.at[o_rows(me)]),
    ]
    loads = [pltpu.make_async_copy(a, b, own_sem.at[i]) for i, (a, b) in enumerate(loads)]
    for one in loads:
        one.start()
    go(s_first[:2] + o_first + s_first[2:] + gains)
    for one in loads:
        one.wait()
    go(first_out)

    summarise(k_ref, v_ref, in_ref, fg_ref, gates_ref, st_ref)
    swap, hand = copy(st_ref, pst_ref, partner), copy(pri_ref, ppri_ref, partner)
    go([swap])
    base = used[0]

    def tell(k):
        return remote(
            cst_ref, gst_ref.at[k - 1], send.at[base + k], recv.at[base + k], chip_at(turn * k)
        )

    def pass_chip_state():
        swap.wait_recv()
        top, f1, f2 = merged((st_ref[272:280],), (pst_ref[272:280], pst_ref[280:288]))
        side = pl.ds(136 * core, 136)
        own_state, next_state = st_ref[side], pst_ref[side]
        t1, l1 = spread_rows(f1, core)
        t2, l2 = spread_rows(f2, core)
        cst_ref[0:128] = t1 * own_state[:128] + t2 * next_state[:128]
        cst_ref[128:136] = l1 * own_state[128:] + l2 * next_state[128:]
        cst_ref[136:144] = top
        cst_ref[144:152] = st_ref[280:288] + pst_ref[280:288]
        for k in range(1, chips):

            @pl.when(place + k < chips)
            def _():
                tell(k).start()

    def collect_states():
        def listen(k, carry):
            acc, peak = carry
            tell(k).wait_recv()
            scale = gst_ref[k - 1, 136:144] + acc
            lw_ref[k - 1] = scale
            return acc + gst_ref[k - 1, 144:152], jnp.maximum(peak, scale)

        none = jnp.full((8, 128), VERY_LOW, F32)
        _, peak = lax.fori_loop(1, place + 1, listen, (jnp.zeros((8, 128), F32), none))

        def gather(k, carry):
            matrix, norm = carry
            t, l = spread_rows(jnp.exp(lw_ref[k - 1] - peak), core)
            return matrix + t * gst_ref[k - 1, 0:128], norm + l * gst_ref[k - 1, 128:136]

        matrix, norm = lax.fori_loop(
            1, place + 1, gather, (jnp.zeros((128, 128), F32), jnp.zeros((8, 128), F32))
        )
        pri_ref[0:128] = matrix
        pri_ref[128:136] = norm
        pri_ref[136:144] = peak
        go([hand])

    def between(j):
        if j == 0:
            pass_chip_state()
            arrive(first_out)
            go(first_on + direct[0])
        elif j == 1:
            arrive(s_first[:2])
            go(s_next)
            go(direct[1])
        elif j == 2:
            arrive(first_on)
            go(direct[2])
        elif j == 3:
            arrive(o_first)
            go(o_next + o_over[:2])
            arrive(direct[0])
            go(onward[0])
        elif j == 4:
            collect_states()

    attend_local(q_ref, k_ref, v_ref, gates_ref, own_ref, res_ref, vx_ref, between)

    hand.wait_recv()
    top, f1, f2 = merged((ppri_ref[136:144],), (pst_ref[272:280], pst_ref[280:288]))
    t1, l1 = spread_rows(f1, 1 - core)
    t2, l2 = spread_rows(f2, 1 - core)
    beside = pst_ref[pl.ds(136 * (1 - core), 136)]
    matrix2 = t1 * ppri_ref[0:128] + t2 * beside[:128]
    norm2 = l1 * ppri_ref[128:136] + l2 * beside[128:]
    matrix, norm, peak = pri_ref[0:128], pri_ref[128:136], pri_ref[136:144]
    zeroth = core == 0
    pair = (
        (jnp.where(zeroth, matrix, matrix2), jnp.where(zeroth, norm, norm2)),
        (jnp.where(zeroth, matrix2, matrix), jnp.where(zeroth, norm2, norm)),
    )
    row = lax.broadcasted_iota(jnp.int32, (8, 128), 0)
    m0 = jnp.where(((row % 4) < 2) == zeroth, peak, top)
    rhs = []
    for mat, nrm in pair:
        wide = jnp.transpose(jnp.broadcast_to(nrm[:1], (128, 128)))
        both = jnp.concatenate([mat, wide], axis=1)
        coarse = both.astype(BF16)
        fine = (both - coarse.astype(F32)).astype(BF16)
        rhs.append(jnp.concatenate([coarse, fine], axis=0))
    turns = [(across, g_first[:2]), (at_right, g_first[2:3]), (at_left, g_first[3:]), (me, [])]
    for at, ready in turns:
        attend_rows(
            pl.multiple_of(at * CHUNK, CHUNK),
            q_ref,
            gates_ref,
            og_ref,
            gain_ref,
            own_ref,
            res_ref,
            gated_ref,
            rhs,
            m0,
        )
        go(ready)
    keep = pltpu.make_async_copy(gated_ref.at[rows_of(me)], gt_ref.at[me], own_sem.at[0])
    keep.start()
    arrive(g_first[:2])
    go(g_next)
    arrive(o_next)
    go(o_over[2:])
    arrive(direct[1])
    go(onward[1])
    arrive(direct[2])
    go(onward[2])
    arrive(s_first[2:] + s_next + gains + o_over + g_first[2:] + g_next)
    keep.wait()

    rows = jnp.concatenate([gt_ref[b] for b in range(TP)], axis=1)
    squares = jnp.zeros((CHUNK, 1), F32)
    for b in range(TP):
        part = dot(rows, ow_all[:, b * WIDE : (b + 1) * WIDE]) + sm_ref[b].astype(F32)
        res_ref[b * CHUNK : (b + 1) * CHUNK] = part
        squares = squares + jnp.sum(part * part, axis=1, keepdims=True)
    scale = lax.rsqrt(squares / D + EPSILON)

    def x_rows(at, start=0, size=PART):
        return pl.ds(pl.multiple_of(at * PART + start, 16), size)

    def ring(i, k, src, dst, to):
        return remote(src, dst, ring_send.at[i, k], ring_recv.at[i, k], to)

    def block_out(k):
        piece = x_ref.at[k, x_rows(me)]
        return ring(0, k, piece, piece, right), ring(1, k, piece, piece, left)

    def block_on(k):
        a = x_ref.at[k, x_rows(at_left, 0, PART // 2)]
        b = x_ref.at[k, x_rows(at_right, PART // 2, PART // 2)]
        return ring(2, k, a, a, right), ring(3, k, b, b, left)

    for k in range(STEPS):
        for b in range(TP):
            part = res_ref[b * CHUNK + k * PART : b * CHUNK + (k + 1) * PART]
            x_ref[k, x_rows(me), b * WIDE : (b + 1) * WIDE] = (
                part * scale[k * PART : (k + 1) * PART] * gn_ref[b][:1]
            ).astype(BF16)
        if k < 2:
            for one in block_out(k):
                one.start()
    for one in block_out(0):
        one.wait_recv()
    for one in block_on(0):
        one.start()
    arrive(sum(onward, []))
    go(over)
    arrive(over)

    def first(k):
        return (
            ring(4, k, half_ref.at[k, 0], got_half.at[k, 0], right),
            ring(5, k, half_ref.at[k, 1], got_half.at[k, 1], left),
        )

    def then(k):
        return (
            ring(6, k, next_ref.at[k, 0], got_next.at[k, 0], right),
            ring(7, k, next_ref.at[k, 1], got_next.at[k, 1], left),
        )

    def block(k, d):
        at = lax.rem(me + d, TP)
        made_ref[...] = dot_t(
            hidden_ref[...], w_ref[pl.ds(pl.multiple_of(at * WIDE, WIDE), WIDE), 2 * HID :]
        )
        rest = pl.ds(pl.multiple_of(at * CHUNK + k * PART, 16), PART)
        made_ref[x_rows(me)] += res_ref[rest]
        return made_ref[...]

    def relay(k):
        for one in first(k):
            one.wait_recv()
        next_ref[k, 0, :, :256] = (
            next_ref[k, 0, :, :256].astype(F32) + got_half[k, 0].astype(F32)
        ).astype(BF16)
        next_ref[k, 1, :, 256:] = (
            next_ref[k, 1, :, 256:].astype(F32) + got_half[k, 1].astype(F32)
        ).astype(BF16)
        for one in then(k):
            one.start()

    def finish(k):
        for one in then(k):
            one.wait_recv()
        for b in range(TP):
            part = pl.ds(b * PART, PART)
            own = own_ref[pl.ds(pl.multiple_of(k * CHUNK + b * PART, 16), PART)]
            out_ref[pl.ds(pl.multiple_of(b * CHUNK + k * PART, 16), PART)] = (
                own + got_next[k, 0, part].astype(F32) + got_next[k, 1, part].astype(F32)
            ).astype(BF16)

    def step(k, carry):
        @pl.when(k + 2 < STEPS)
        def _():
            for one in block_out(k + 2):
                one.start()

        @pl.when(k + 1 < STEPS)
        def _():
            for one in block_out(k + 1):
                one.wait_recv()
            for one in block_on(k + 1):
                one.start()

        for one in block_on(k):
            one.wait_recv()
        x = x_ref[k]
        for i in range(HID // 128):
            both = dot(x, w_ref[:, 256 * i : 256 * i + 256])
            g, u = both[:, :128], both[:, 128:]
            hidden_ref[:, 128 * i : 128 * i + 128] = (g / (1.0 + jnp.exp(-g)) * u).astype(BF16)
        far = block(k, 2).astype(BF16)
        half_ref[k, 0] = far[:, :256]
        half_ref[k, 1] = far[:, 256:]
        for one in first(k):
            one.start()
        next_ref[k, 0] = block(k, 1).astype(BF16)
        next_ref[k, 1] = block(k, 3).astype(BF16)

        @pl.when(k >= 1)
        def _():
            relay(k - 1)

        own_ref[pl.ds(pl.multiple_of(k * CHUNK, CHUNK), CHUNK)] = block(k, 0)

        @pl.when(k >= 2)
        def _():
            finish(k - 2)

        return carry

    lax.fori_loop(0, STEPS, step, 0)
    relay(STEPS - 1)
    finish(STEPS - 2)
    finish(STEPS - 1)
    for one in started:
        one.wait_send()
    for k in range(1, chips):

        @pl.when(place + k < chips)
        def _():
            tell(k).wait_send()

    for k in range(STEPS):
        for one in block_out(k) + block_on(k) + first(k) + then(k):
            one.wait_send()


def local(
    query,
    key_rows,
    value,
    in_gate,
    forget_pre,
    out_gate,
    head_gain,
    out_weight,
    stream,
    norm_gain,
    gate_weight,
    up_weight,
    down_weight,
):
    chips = lax.axis_size("sp") // 2
    n = query.shape[0]
    gain = jnp.broadcast_to(norm_gain.astype(F32)[None], (8, WIDE))
    vmem, anywhere = pl.BlockSpec(memory_space=pltpu.VMEM), pl.BlockSpec(memory_space=pl.ANY)
    dma, tokens = pltpu.SemaphoreType.DMA, TP * CHUNK
    return pl.pallas_call(
        layer_kernel,
        out_shape=jax.ShapeDtypeStruct((tokens, WIDE), BF16),
        in_specs=[vmem] * 8 + [anywhere] * 5,
        out_specs=vmem,
        scratch_shapes=[
            pltpu.VMEM((24, n), F32),
            pltpu.VMEM((288, 128), F32),
            pltpu.VMEM((288, 128), F32),
            pltpu.VMEM((152, 128), F32),
            pltpu.VMEM((max(chips - 1, 1), 152, 128), F32),
            pltpu.VMEM((144, 128), F32),
            pltpu.VMEM((144, 128), F32),
            pltpu.VMEM((max(chips - 1, 1), 8, 128), F32),
            pltpu.VMEM((2, n, 256), BF16),
            pltpu.VMEM((n, 256), BF16),
            pltpu.VMEM((TP, CHUNK, 256), BF16),
            pltpu.VMEM((2, HALF, 256), BF16),
            pltpu.VMEM((TP, CHUNK, WIDE), BF16),
            pltpu.VMEM((2, HALF, WIDE), BF16),
            pltpu.VMEM((TP, 8, WIDE), F32),
            pltpu.VMEM((1024, D), BF16),
            pltpu.VMEM((tokens, WIDE), F32),
            pltpu.VMEM((tokens, WIDE), F32),
            pltpu.VMEM((D, 3 * HID), BF16),
            pltpu.VMEM((STEPS, CHUNK, D), BF16),
            pltpu.VMEM((CHUNK, HID), BF16),
            pltpu.VMEM((CHUNK, WIDE), F32),
            pltpu.VMEM((STEPS, 2, CHUNK, 256), BF16),
            pltpu.VMEM((STEPS, 2, CHUNK, WIDE), BF16),
            pltpu.VMEM((STEPS, 2, CHUNK, 256), BF16),
            pltpu.VMEM((STEPS, 2, CHUNK, WIDE), BF16),
            dma((120,)),
            dma((120,)),
            dma((8, STEPS)),
            dma((8, STEPS)),
            dma((32,)),
        ],
        compiler_params=pltpu.CompilerParams(
            collective_id=1, has_side_effects=True, vmem_limit_bytes=67043328
        ),
        cost_estimate=pl.CostEstimate(
            flops=90_000_000_000, bytes_accessed=20_000_000, transcendentals=0
        ),
        name="layer",
    )(
        query,
        key_rows,
        value,
        in_gate,
        forget_pre,
        out_gate,
        head_gain.reshape(1, 256),
        gain,
        stream,
        out_weight,
        gate_weight,
        up_weight,
        down_weight,
    )


def solution(mesh):
    placed = (
        P("sp", "tp"),
        P("sp", "tp"),
        P("sp", "tp"),
        P(None, "tp", "sp"),
        P(None, "tp", "sp"),
        P("sp", "tp"),
        P("tp"),
        P("tp", None),
        P("sp", "tp"),
        P("tp"),
        P("sp", "tp"),
        P("sp", "tp"),
        P("sp", "tp"),
    )
    return jax.shard_map(
        local, mesh=mesh, in_specs=placed, out_specs=P("sp", "tp"), check_vma=False
    )
```
